32 devices in a mesh: ep: 8 (over z, x), tp: 4 (over y, core).
Axes of the slice: x: 2, y: 2, z: 4, core: 2. Of those that a mesh axis runs over, the one named last changes fastest.
Arguments:
- pool_input: bfloat16 [4096, 1024], P('ep', 'tp'), may hold values from -6 to 6
- group_weight: bfloat16 [4, 256, 256], P('tp'), may hold values from -0.375 to 0.375
- pool_scale: float32 [1024], P('tp'), may hold values from 0.1 to 1.9
- out_weight: bfloat16 [1024, 2048], P('tp'), may hold values from -0.1875 to 0.1875
- mix_gain: float32 [2048], replicated, may hold values from 0.1 to 1.9
- expert_input: bfloat16 [8192, 2048], P(('ep', 'tp')), may hold values from -6 to 6
- routes: int32 [8192, 2], P('ep'), may hold values from 0 to 15, all different within a row; in each aligned block of 256 rows (0 to 255, 256 to 511, ...) at most 40 rows name the same one
- route_weights: float32 [8192, 2], P('ep'), may hold values from 0.2 to 2.5
- moe_in_gain: float32 [2048], replicated, may hold values from 0.1 to 1.9
- gate_weight: bfloat16 [16, 2048, 1024], P('ep', None, 'tp'), may hold values from -0.125 to 0.125
- up_weight: bfloat16 [16, 2048, 1024], P('ep', None, 'tp'), may hold values from -0.125 to 0.125
- down_weight: bfloat16 [16, 1024, 2048], P('ep', 'tp'), may hold values from -0.1875 to 0.1875
- moe_out_gain: float32 [2048], replicated, may hold values from 0.1 to 1.9
Outputs:
- mixer_out: bfloat16 [4096, 2048], P(('ep', 'tp'))
- moe_out: bfloat16 [8192, 2048], P(('ep', 'tp'))
The draws below stay inside these ranges and needn't reach their ends.
Inputs may be any that keep to these rules, and one draw needn't show every extreme that they name: `routes`: each row names 2 different experts. In each aligned block of 256 rows no expert is named by more than 40 rows, a bound that some block reaches.
All inputs are finite; a program needn't handle non-finite values.
Results may differ from the reference program's by a relative error of at most 0.013.
Values may be sent and summed in bfloat16 or wider, within the bound.
A program may use at most 128 MiB of HBM per device.

```python
import math
from functools import partial
import jax
import jax.numpy as jnp
import numpy as np
from jax import lax

D = 2048
GROUPS = 4
GW = 256
PW = 1024
FF = 1024
FF_BLK = 256
EXPERTS = 16
TOPK = 2
TOKB_DEV = 256
CAP = 40
TOKENS_A = 4096
TOKENS_B = 8192
N_TP = 4


def block_levels(key, shape, shards, smallest, high):
    gain, own = 1.0, jax.random.fold_in(key, 6)
    for dim, blocks in shards:
        steps = jnp.exp(jax.random.uniform(jax.random.fold_in(own, dim), (blocks,), jnp.float32, smallest / len(shards), high / len(shards)))
        gain = gain * jnp.repeat(steps, shape[dim] // blocks).reshape([-1 if axis == dim else 1 for axis in range(len(shape))])
    return gain


def deal_out(key, own, number, rows, number_of, top, most, slope):
    ranking = jax.random.permutation(key, number_of)
    crowded, usual = shares(number_of, rows * top, most, slope, True), shares(number_of, rows * top, most, slope, False)
    places = jnp.arange(number_of)

    def named(sizes, rotation):
        used = int((sizes > 0).sum())
        fixed = max(1, used // 4)
        passed = fixed + (places - fixed + rotation * (used - fixed)) % max(1, number_of - fixed)
        return jnp.zeros((number_of,), jnp.int32).at[ranking[jnp.where(places < fixed, places, passed)]].set(jnp.asarray(sizes, jnp.int32))

    sizes = jnp.where(number % 4 == 0, named(crowded, number // 4), named(usual, number - number // 4 - 1))
    mixed = jax.random.permutation(jax.random.fold_in(own, 3), number_of)
    donor, sink = mixed[0:number_of // 2 * 2:2], mixed[1:number_of // 2 * 2:2]
    margin = jnp.minimum(sizes[donor] - 1, most - sizes[sink]) // 2
    margin = jnp.where((donor == ranking[0]) | (sink == ranking[0]) | (sizes[sink] == 0), 0, jnp.maximum(margin, 0))
    passed = jax.random.randint(jax.random.fold_in(own, 4), (number_of // 2,), 0, 1 << 20) % (margin + 1)
    sizes = sizes.at[donor].add(-passed).at[sink].add(passed)
    items = jnp.searchsorted(jnp.cumsum(sizes), jnp.arange(rows * top), side="right").astype(jnp.int32)
    grid = items.reshape(top, rows).T
    grid = grid[jax.random.permutation(jax.random.fold_in(own, 1), rows)]
    rotation = jax.random.randint(jax.random.fold_in(own, 2), (rows, 1), 0, top)
    return jnp.take_along_axis(grid, (jnp.arange(top)[None, :] + rotation) % top, axis=1)


def shares(number_of, total, bound, skew, full):
    portions = [(1 << 20) // math.isqrt(rank ** skew) + 1 for rank in range(1, number_of + 1)]
    largest = bound if full else min(bound, max(-(-total // number_of), total * portions[0] // sum(portions)))
    least = 1 if total - largest >= number_of - 1 else 0
    given, rest = [largest] + [least] * (number_of - 1), total - largest - least * (number_of - 1)
    while rest > 0:
        movable = [i for i in range(1, number_of) if given[i] < largest] or [i for i in range(1, number_of) if given[i] < bound]
        whole, remaining = sum([portions[i] for i in movable]), rest
        for i in movable:
            more = min(bound - given[i], max(1, remaining * portions[i] // whole), rest)
            given[i] = given[i] + more
            rest = rest - more
    return np.array(given)


def scatter_about(own_key, dims, scale, bound, split=(), kind=jnp.bfloat16):
    entries = scale * jax.random.normal(own_key, dims, jnp.float32)
    if split:
        entries = entries * block_levels(own_key, dims, split, -0.22, 0.18)
    return jnp.clip(entries, -bound, bound).astype(kind)


def setup_inputs(seed: int = 0) -> dict:
    key_list = jax.random.split(jax.random.key(seed), 14)
    pool_input = scatter_about(key_list[0], (TOKENS_A, PW), 1.0, 6.0, ((0, 8), (1, 4)))
    group_weight = scatter_about(key_list[1], (GROUPS, GW, GW), GW ** -0.5, 0.375, ((0, 4),))
    pool_scale = jnp.clip(1.0 + 0.18 * jax.random.normal(key_list[2], (PW,), jnp.float32), 0.1, 1.9)
    out_weight = scatter_about(key_list[3], (PW, D), PW ** -0.5, 0.1875, ((0, 4),))
    mix_gain = jnp.clip(1.0 + 0.18 * jax.random.normal(key_list[4], (D,), jnp.float32), 0.1, 1.9)
    expert_input = scatter_about(key_list[5], (TOKENS_B, D), 1.0, 6.0, ((0, 32),))
    routes_keys = jax.random.split(jax.random.fold_in(key_list[6], 1), TOKENS_B // TOKB_DEV)
    routes_turns = jax.random.permutation(jax.random.fold_in(key_list[6], 3), TOKENS_B // TOKB_DEV)
    routes = jax.vmap(lambda own, number: deal_out(jax.random.fold_in(key_list[6], 2), own, number, TOKB_DEV, EXPERTS, TOPK, CAP, 1))(routes_keys, routes_turns).reshape((TOKENS_B, TOPK))
    route_weights = jnp.clip(jnp.exp(math.log(2.5) - 2.5257286 * jax.random.uniform(key_list[7], (TOKENS_B, TOPK), jnp.float32) ** block_levels(key_list[7], (TOKENS_B, TOPK), ((0, 8),), -0.2, 0.2)), 0.2, 2.5)
    moe_in_gain = jnp.clip(1.0 + 0.18 * jax.random.normal(key_list[8], (D,), jnp.float32), 0.1, 1.9)
    gate_weight = scatter_about(key_list[9], (EXPERTS, D, FF), D ** -0.5, 0.125, ((0, 8), (2, 4)))
    up_weight = scatter_about(key_list[10], (EXPERTS, D, FF), D ** -0.5, 0.125, ((0, 8), (2, 4)))
    down_weight = scatter_about(key_list[11], (EXPERTS, FF, D), FF ** -0.5, 0.1875, ((0, 8), (1, 4)))
    moe_out_gain = jnp.clip(1.0 + 0.18 * jax.random.normal(key_list[12], (D,), jnp.float32), 0.1, 1.9)
    return {"pool_input": pool_input, "group_weight": group_weight, "pool_scale": pool_scale, "out_weight": out_weight, "mix_gain": mix_gain, "expert_input": expert_input, "routes": routes, "route_weights": route_weights, "moe_in_gain": moe_in_gain, "gate_weight": gate_weight, "up_weight": up_weight, "down_weight": down_weight, "moe_out_gain": moe_out_gain}


NORM_EPS = 1e-06

def rms_scale(values, gain_vec):
    mean_sq = lax.optimization_barrier(jnp.mean(values * values, axis=-1, keepdims=True))
    return values * lax.rsqrt(mean_sq + NORM_EPS) * gain_vec.astype(jnp.float32)

def pool_group(block_in, window):
    row_total = block_in.shape[0]
    values = block_in.astype(jnp.float32)
    padded = jnp.pad(values, ((window - 1, 0), (0, 0)))
    summed = jnp.zeros_like(values)
    for lag_step in range(window):
        summed = summed + padded[window - 1 - lag_step:window - 1 - lag_step + row_total]
    divisor = jnp.minimum(jnp.arange(row_total) + 1, window).astype(jnp.float32)[:, None]
    return (summed / divisor - values).astype(jnp.bfloat16)

def slot_numbers(route_block, experts, capacity):
    flat_routes = route_block.reshape(-1).astype(jnp.int32)
    one_hot = (flat_routes[:, None] == jnp.arange(experts, dtype=jnp.int32)[None, :]).astype(jnp.int32)
    slot_rank = lax.optimization_barrier(jnp.sum((jnp.cumsum(one_hot, axis=0) - one_hot) * one_hot, axis=1))
    return (flat_routes * capacity + slot_rank).astype(jnp.int32)

def fill_table(slot_ids, payload, empty_value, slots_total):
    return jnp.full((slots_total,), empty_value, payload.dtype).at[slot_ids].set(payload)

def reference(pool_input, group_weight, pool_scale, out_weight, mix_gain, expert_input, routes, route_weights, moe_in_gain, gate_weight, up_weight, down_weight, moe_out_gain):
    projected = jnp.zeros((TOKENS_A, D), jnp.float32)
    for group_idx in range(GROUPS):
        lo_col = group_idx * GW
        pooled = pool_group(pool_input[:, lo_col:lo_col + GW], 2 ** (group_idx + 1))
        grouped = (jnp.dot(pooled, group_weight[group_idx], preferred_element_type=jnp.float32) * pool_scale[lo_col:lo_col + GW].astype(jnp.float32)).astype(jnp.bfloat16)
        partial_mix = jnp.dot(grouped, out_weight[lo_col:lo_col + GW], preferred_element_type=jnp.float32).astype(jnp.bfloat16)
        projected = projected + partial_mix.astype(jnp.float32)
    mixer_out = rms_scale(projected, mix_gain).astype(jnp.bfloat16)
    normed = rms_scale(expert_input.astype(jnp.float32), moe_in_gain).astype(jnp.bfloat16)
    blocks = TOKENS_B // TOKB_DEV
    pairs = TOKB_DEV * TOPK
    route_blocks = routes.reshape(blocks, TOKB_DEV, TOPK)
    slot_ids = jax.vmap(partial(slot_numbers, experts=EXPERTS, capacity=CAP))(route_blocks)
    pair_token = (jnp.arange(blocks, dtype=jnp.int32)[:, None] * TOKB_DEV + jnp.arange(pairs, dtype=jnp.int32)[None, :] // TOPK).astype(jnp.int32)
    token_table = jax.vmap(partial(fill_table, empty_value=TOKENS_B, slots_total=EXPERTS * CAP))(slot_ids, pair_token)
    weight_table = jax.vmap(partial(fill_table, empty_value=0.0, slots_total=EXPERTS * CAP))(slot_ids, route_weights.reshape(blocks, pairs))
    token_table = token_table.reshape(blocks, EXPERTS, CAP).transpose(1, 0, 2).reshape(EXPERTS, blocks * CAP)
    weight_table = weight_table.reshape(blocks, EXPERTS, CAP).transpose(1, 0, 2).reshape(EXPERTS, blocks * CAP)
    padded_rows = jnp.concatenate([normed, jnp.zeros((1, D), jnp.bfloat16)], axis=0)

    def run_expert(combined, expert_inputs):
        token_idx, slot_weight, w_gate, w_up, w_down = expert_inputs
        gathered = padded_rows[token_idx]
        gate_act = jnp.dot(gathered, w_gate, preferred_element_type=jnp.float32)
        up_act = jnp.dot(gathered, w_up, preferred_element_type=jnp.float32)
        hidden = (jax.nn.silu(gate_act) * up_act).astype(jnp.bfloat16)
        block_parts = jnp.einsum('rjf,jfd->jrd', hidden.reshape(-1, N_TP, FF_BLK).astype(jnp.float32), w_down.reshape(N_TP, FF_BLK, D).astype(jnp.float32)).astype(jnp.bfloat16)
        expert_out = lax.optimization_barrier(jnp.sum(block_parts.astype(jnp.float32), axis=0)).astype(jnp.bfloat16)
        combined = combined.at[token_idx].add(slot_weight[:, None] * expert_out.astype(jnp.float32))
        return (combined, None)
    start_sums = jnp.zeros((TOKENS_B + 1, D), jnp.float32)
    combined, ignored = lax.scan(run_expert, start_sums, (token_table, weight_table, gate_weight, up_weight, down_weight))
    moe_out = rms_scale(combined[:TOKENS_B], moe_out_gain).astype(jnp.bfloat16)
    return (mixer_out, moe_out)
```

```python
import functools

import jax
import jax.numpy as jnp
from jax import lax
from jax.experimental import pallas as pl
from jax.experimental.pallas import tpu as pltpu
from jax.sharding import PartitionSpec as P

NORM_EPS = 1e-06


def passed_along(value, axis, steps):
    count = lax.axis_size(axis)
    initial, last = (max(0, -steps), min(count, count - steps))
    return lax.ppermute(value, axis, [(source, source + steps) for source in range(initial, last)])


def rms_scale(values, gain_vec):
    mean_sq = jnp.mean(values * values, axis=-1, keepdims=True)
    return values * lax.rsqrt(mean_sq + NORM_EPS) * gain_vec


def slot_numbers(route_block, experts, capacity, exp_dev, block_rows):
    flat_routes = route_block.reshape(-1)
    one_hot = (flat_routes[:, None] == jnp.arange(experts, dtype=jnp.int32)[None, :]).astype(
        jnp.int32
    )
    slot_rank = jnp.sum((jnp.cumsum(one_hot, axis=0) - one_hot) * one_hot, axis=1)
    owner = flat_routes // exp_dev
    local = flat_routes - owner * exp_dev
    return owner * block_rows + local * capacity + slot_rank


def fill_table(slot_ids, payload, empty_value, slots_total):
    return jnp.full((slots_total,), empty_value, payload.dtype).at[slot_ids].set(payload)


MESH = pl.DeviceIdType.MESH


def exchange_kernel(
    capacity,
    outgoing,
    mix_part,
    gate_hbm,
    up_hbm,
    down_hbm,
    returned,
    projected,
    arrived,
    part,
    core_in,
    chip_sum,
    cross_in,
    final,
    gate,
    up,
    down,
    mix_held,
    mix_core,
    mix_sum,
    mix_cross,
    local_sem,
    dis_send,
    dis_recv,
    y1_send,
    y1_recv,
    c1_send,
    c1_recv,
    c2_send,
    c2_recv,
    y2_send,
    y2_recv,
    ret_send,
    ret_recv,
    m1_send,
    m1_recv,
    m2_send,
    m2_recv,
):
    ep_size, tp_size, rows, width = arrived.shape
    exp_dev, _, ff_dev = gate.shape
    highs = tp_size // 2
    ep = lax.axis_index("ep")
    tp = lax.axis_index("tp")
    hi, lo = tp // 2, tp % 2
    other = 1 - lo

    def remote(src, dst, send, recv, to_ep, to_tp):
        return pltpu.make_async_remote_copy(
            src_ref=src,
            dst_ref=dst,
            send_sem=send,
            recv_sem=recv,
            device_id=(to_ep, to_tp),
            device_id_type=MESH,
        )

    def peer_high(k):
        return lax.rem(hi + k, highs)

    def offset_of(i):
        return jnp.where(i < 2, i, ep_size + 1 - i)

    def partner_ep(d):
        low = d
        mine = ep
        value = ep * 0
        bit = 1
        while bit < ep_size:
            a = (mine // bit) % 2
            b = (low // bit) % 2
            value = value + bit * ((a + b) % 2)
            bit *= 2
        return value

    def dispatch(d):
        peer = partner_ep(d)
        return remote(
            outgoing.at[peer], arrived.at[d, tp], dis_send.at[d], dis_recv.at[d], peer, tp
        )

    def gather_cross(d, k):
        high = peer_high(k)
        return remote(
            arrived.at[d, tp],
            arrived.at[d, tp],
            y1_send.at[d, k],
            y1_recv.at[d, highs - k],
            ep,
            high * 2 + lo,
        )

    def gather_cross_in(d, k):
        high = peer_high(k)
        return remote(
            arrived.at[d, high * 2 + lo],
            arrived.at[d, high * 2 + lo],
            y1_send.at[d, k],
            y1_recv.at[d, k],
            ep,
            high * 2 + lo,
        )

    def gather_core(d, high):
        slot = arrived.at[d, high * 2 + lo]
        return remote(slot, slot, c1_send.at[d, high], c1_recv.at[d, high], ep, hi * 2 + other)

    def gather_core_in(d, high):
        slot = arrived.at[d, high * 2 + other]
        return remote(slot, slot, c1_send.at[d, high], c1_recv.at[d, high], ep, hi * 2 + other)

    def reduce_core(d, high):
        return remote(
            part.at[high * 2 + other],
            core_in.at[d, high],
            c2_send.at[d, high],
            c2_recv.at[d, high],
            ep,
            hi * 2 + other,
        )

    def reduce_cross(d, k):
        high = peer_high(k)
        return remote(
            chip_sum.at[high],
            cross_in.at[d, highs - k - 1],
            y2_send.at[d, k],
            y2_recv.at[d, highs - k],
            ep,
            high * 2 + lo,
        )

    def reduce_cross_in(d, k):
        high = peer_high(k)
        return remote(
            chip_sum.at[high],
            cross_in.at[d, k - 1],
            y2_send.at[d, k],
            y2_recv.at[d, k],
            ep,
            high * 2 + lo,
        )

    def give_back(d):
        peer = partner_ep(d)
        return remote(final.at[d], returned.at[ep], ret_send.at[d], ret_recv.at[d], peer, tp)

    def give_back_in(d):
        peer = partner_ep(d)
        return remote(final.at[d], returned.at[peer], ret_send.at[d], ret_recv.at[d], peer, tp)

    def mix_core_copy(high):
        return remote(
            mix_held.at[high * 2 + other],
            mix_core.at[high],
            m1_send.at[high],
            m1_recv.at[high],
            ep,
            hi * 2 + other,
        )

    def mix_cross_copy(k):
        high = peer_high(k)
        return remote(
            mix_sum.at[high],
            mix_cross.at[highs - k - 1],
            m2_send.at[k],
            m2_recv.at[highs - k],
            ep,
            high * 2 + lo,
        )

    def mix_cross_in(k):
        high = peer_high(k)
        return remote(
            mix_sum.at[high],
            mix_cross.at[k - 1],
            m2_send.at[k],
            m2_recv.at[k],
            ep,
            high * 2 + lo,
        )

    own_rows = pltpu.make_async_copy(outgoing.at[ep], arrived.at[0, tp], local_sem.at[0])
    own_mix = pltpu.make_async_copy(mix_part, mix_held, local_sem.at[1])
    weight_copies = [
        pltpu.make_async_copy(gate_hbm, gate, local_sem.at[2]),
        pltpu.make_async_copy(up_hbm, up, local_sem.at[3]),
        pltpu.make_async_copy(down_hbm, down, local_sem.at[4]),
    ]
    own_rows.start()
    own_mix.start()
    for copy in weight_copies:
        copy.start()

    barrier = pltpu.get_barrier_semaphore()

    def greet(d, carry):
        pl.semaphore_signal(barrier, inc=1, device_id=(partner_ep(d), tp), device_id_type=MESH)
        return carry

    lax.fori_loop(1, ep_size, greet, 0)
    for k in range(1, highs):
        pl.semaphore_signal(
            barrier, inc=1, device_id=(ep, peer_high(k) * 2 + lo), device_id_type=MESH
        )
    pl.semaphore_signal(barrier, inc=1, device_id=(ep, hi * 2 + other), device_id_type=MESH)
    pl.semaphore_wait(barrier, ep_size - 1 + highs)

    def send_out(i, carry):
        dispatch(offset_of(i)).start()
        return carry

    lax.fori_loop(1, ep_size, send_out, 0)

    def stage_a(d):
        for k in range(1, highs):
            gather_cross(d, k).start()
        gather_core(d, hi).start()

    own_rows.wait()
    stage_a(0)

    own_mix.wait()
    for high in range(highs):
        mix_core_copy(high).start()
    for high in range(highs):
        mix_core_copy(high).wait_recv()
    for high in range(highs):
        mix_sum[high] = (
            mix_held[high * 2 + lo].astype(jnp.float32) + mix_core[high].astype(jnp.float32)
        ).astype(jnp.bfloat16)
    for k in range(1, highs):
        mix_cross_copy(k).start()
    for copy in weight_copies:
        copy.wait()

    row_expert = (
        lax.rem(lax.broadcasted_iota(jnp.int32, (tp_size * rows, 1), 0), rows) // capacity
    )
    column_step = min(width, 512)

    def step(i, carry):
        @pl.when(i + 1 < ep_size)
        def _():
            d = offset_of(i + 1)
            dispatch(d).wait_recv()
            stage_a(d)

        @pl.when(i < ep_size)
        def _():
            d = offset_of(i)
            for k in range(1, highs):
                gather_cross_in(d, k).wait_recv()
                gather_core(d, peer_high(k)).start()

        @pl.when(i >= 2)
        def _():
            d = offset_of(i - 2)
            total = chip_sum[hi].astype(jnp.float32)
            for k in range(1, highs):
                reduce_cross(d, k).wait_send()
                reduce_cross_in(d, k).wait_recv()
                total = total + cross_in[d, k - 1].astype(jnp.float32)
            final[d] = total.astype(jnp.bfloat16)

            @pl.when(i == 2)
            def _():
                pltpu.make_async_copy(final.at[0], returned.at[ep], local_sem.at[0]).start()

            @pl.when(i > 2)
            def _():
                give_back(d).start()

        @pl.when((i >= 1) & (i <= ep_size))
        def _():
            d = offset_of(i - 1)
            for high in range(highs):
                reduce_core(d, high).wait_recv()
                reduce_core(d, high).wait_send()
                chip_sum[high] = (
                    part[high * 2 + lo].astype(jnp.float32) + core_in[d, high].astype(jnp.float32)
                ).astype(jnp.bfloat16)
            for k in range(1, highs):
                reduce_cross(d, k).start()

        @pl.when(i < ep_size)
        def _():
            d = offset_of(i)
            for high in range(highs):
                gather_core_in(d, high).wait_recv()
            hidden = []
            for e in range(exp_dev):
                block = arrived[d].reshape(tp_size * rows, width)
                gate_act = jnp.dot(block, gate[e], preferred_element_type=jnp.float32)
                up_act = jnp.dot(block, up[e], preferred_element_type=jnp.float32)
                act = gate_act / (1.0 + jnp.exp(-gate_act)) * up_act
                hidden.append(jnp.where(row_expert == e, act, 0.0).astype(jnp.bfloat16))
            joined = jnp.concatenate(hidden, axis=1)
            for start in range(0, width, column_step):
                columns = slice(start, start + column_step)
                out = jnp.dot(
                    joined,
                    down[:, :, columns].reshape(exp_dev * ff_dev, column_step),
                    preferred_element_type=jnp.float32,
                )
                part[:, :, columns] = out.astype(jnp.bfloat16).reshape(tp_size, rows, column_step)
            for high in range(highs):
                reduce_core(d, high).start()

        return carry

    lax.fori_loop(0, ep_size + 2, step, 0)

    total = mix_sum[hi].astype(jnp.float32)
    for k in range(1, highs):
        mix_cross_in(k).wait_recv()
        total = total + mix_cross[k - 1].astype(jnp.float32)
    projected[...] = total
    for k in range(1, highs):
        mix_cross_copy(k).wait_send()
    for high in range(highs):
        mix_core_copy(high).wait_send()

    def drain_all(d, carry):
        for k in range(1, highs):
            gather_cross(d, k).wait_send()
        for high in range(highs):
            gather_core(d, high).wait_send()
        return carry

    lax.fori_loop(0, ep_size, drain_all, 0)

    def drain(i, carry):
        d = offset_of(i)
        dispatch(d).wait_send()
        give_back(d).wait_send()
        give_back_in(d).wait_recv()
        return carry

    lax.fori_loop(1, ep_size, drain, 0)
    pltpu.make_async_copy(final.at[0], returned.at[ep], local_sem.at[0]).wait()


def exchange(outgoing, mix_part, gate_weight, up_weight, down_weight, capacity):
    ep_size, rows, width = outgoing.shape
    tp_size, mix_rows, _ = mix_part.shape
    highs = tp_size // 2
    bf16 = jnp.bfloat16
    any_spec = pl.BlockSpec(memory_space=pl.ANY)
    dma = pltpu.SemaphoreType.DMA
    pair = (ep_size, highs)
    flops = 6 * gate_weight.size * ep_size * tp_size * rows
    return pl.pallas_call(
        functools.partial(exchange_kernel, capacity),
        out_shape=(
            jax.ShapeDtypeStruct(outgoing.shape, bf16),
            jax.ShapeDtypeStruct((mix_rows, width), jnp.float32),
        ),
        in_specs=[any_spec] * 5,
        out_specs=(any_spec, pl.BlockSpec(memory_space=pltpu.VMEM)),
        scratch_shapes=[
            pltpu.VMEM((ep_size, tp_size, rows, width), bf16),
            pltpu.VMEM((tp_size, rows, width), bf16),
            pltpu.VMEM((ep_size, highs, rows, width), bf16),
            pltpu.VMEM((highs, rows, width), bf16),
            pltpu.VMEM((ep_size, highs - 1, rows, width), bf16),
            pltpu.VMEM((ep_size, rows, width), bf16),
            pltpu.VMEM(gate_weight.shape, bf16),
            pltpu.VMEM(up_weight.shape, bf16),
            pltpu.VMEM(down_weight.shape, bf16),
            pltpu.VMEM(mix_part.shape, bf16),
            pltpu.VMEM((highs, mix_rows, width), bf16),
            pltpu.VMEM((highs, mix_rows, width), bf16),
            pltpu.VMEM((highs - 1, mix_rows, width), bf16),
            dma((5,)),
            dma((ep_size,)),
            dma((ep_size,)),
            dma(pair),
            dma(pair),
            dma(pair),
            dma(pair),
            dma(pair),
            dma(pair),
            dma(pair),
            dma(pair),
            dma((ep_size,)),
            dma((ep_size,)),
            dma((highs,)),
            dma((highs,)),
            dma((highs,)),
            dma((highs,)),
        ],
        compiler_params=pltpu.CompilerParams(
            collective_id=0, has_side_effects=True, vmem_limit_bytes=60 * 1024 * 1024
        ),
        cost_estimate=pl.CostEstimate(
            flops=flops, bytes_accessed=4 * outgoing.size, transcendentals=0
        ),
    )(outgoing, mix_part, gate_weight, up_weight, down_weight)


def on_device(
    pool_input,
    group_weight,
    pool_scale,
    out_weight,
    mix_gain,
    expert_input,
    routes,
    route_weights,
    moe_in_gain,
    gate_weight,
    up_weight,
    down_weight,
    moe_out_gain,
):
    tp_size = lax.axis_size("tp")
    ep_size = lax.axis_size("ep")
    tp_index = lax.axis_index("tp")
    rows_a = pool_input.shape[0]
    model_width = out_weight.shape[1]
    history_rows = 2**tp_size
    window = jnp.left_shift(jnp.int32(2), tp_index)
    history = passed_along(pool_input[rows_a - history_rows :], "ep", 1)
    extended = jnp.concatenate([history, pool_input], axis=0).astype(jnp.float32)
    running = jnp.cumsum(extended, axis=0)
    lagged = lax.dynamic_slice_in_dim(running, history_rows - window, rows_a, 0)
    current = running[history_rows:]
    position = lax.axis_index("ep") * rows_a + jnp.arange(rows_a, dtype=jnp.int32)
    divisor = jnp.minimum(position + 1, window).astype(jnp.float32)[:, None]
    pooled = ((current - lagged) / divisor - extended[history_rows:]).astype(jnp.bfloat16)
    grouped = (
        jnp.dot(pooled, group_weight[0], preferred_element_type=jnp.float32) * pool_scale
    ).astype(jnp.bfloat16)
    exp_dev = gate_weight.shape[0]
    experts = exp_dev * ep_size
    tok_dev = expert_input.shape[0]
    top_count = routes.shape[1]
    capacity = max(2, 5 * tok_dev * top_count // (4 * experts))
    block_rows = -(-exp_dev * capacity // 16) * 16
    slots_total = ep_size * block_rows
    normed = rms_scale(expert_input.astype(jnp.float32), moe_in_gain).astype(jnp.bfloat16)
    own_routes = lax.dynamic_slice_in_dim(routes, tp_index * tok_dev, tok_dev, 0)
    own_slots = slot_numbers(own_routes, experts, capacity, exp_dev, block_rows)
    pair_token = jnp.arange(tok_dev * top_count, dtype=jnp.int32) // top_count
    token_table = fill_table(own_slots, pair_token, tok_dev, slots_total)
    padded_rows = jnp.concatenate([normed, jnp.zeros((1, model_width), jnp.bfloat16)], axis=0)
    outgoing = padded_rows[token_table].reshape(ep_size, block_rows, model_width)
    mix_part = (
        jnp.dot(grouped, out_weight, preferred_element_type=jnp.float32)
        .astype(jnp.bfloat16)
        .reshape(tp_size, rows_a // tp_size, model_width)
    )
    returned, projected = exchange(
        outgoing, mix_part, gate_weight, up_weight, down_weight, capacity
    )
    mixer_out = rms_scale(projected, mix_gain).astype(jnp.bfloat16)
    back = returned.reshape(slots_total, model_width)
    slot_pairs = own_slots.reshape(tok_dev, top_count)
    own_weights = lax.dynamic_slice_in_dim(route_weights, tp_index * tok_dev, tok_dev, 0)
    combined = jnp.zeros((tok_dev, model_width), jnp.float32)
    for k in range(top_count):
        combined = combined + back[slot_pairs[:, k]].astype(jnp.float32) * own_weights[:, k : k + 1]
    moe_out = rms_scale(combined, moe_out_gain).astype(jnp.bfloat16)
    return (mixer_out, moe_out)


def solution(mesh):
    in_specs = (
        P("ep", "tp"),
        P("tp", None, None),
        P("tp"),
        P("tp", None),
        P(),
        P(("ep", "tp"), None),
        P("ep", None),
        P("ep", None),
        P(),
        P("ep", None, "tp"),
        P("ep", None, "tp"),
        P("ep", "tp", None),
        P(),
    )
    out_specs = (P(("ep", "tp"), None), P(("ep", "tp"), None))
    return jax.shard_map(
        on_device, mesh=mesh, in_specs=in_specs, out_specs=out_specs, check_vma=False
    )
```

```python
import functools

import jax
import jax.numpy as jnp
from jax import lax
from jax.experimental import pallas as pl
from jax.experimental.pallas import tpu as pltpu
from jax.sharding import PartitionSpec as P

NORM_EPS = 1e-06


def passed_along(value, axis, steps):
    count = lax.axis_size(axis)
    initial, last = (max(0, -steps), min(count, count - steps))
    return lax.ppermute(value, axis, [(source, source + steps) for source in range(initial, last)])


def rms_scale(values, gain_vec):
    mean_sq = jnp.mean(values * values, axis=-1, keepdims=True)
    return values * lax.rsqrt(mean_sq + NORM_EPS) * gain_vec


def slot_numbers(route_block, experts, capacity, exp_dev, block_rows):
    flat_routes = route_block.reshape(-1)
    one_hot = (flat_routes[:, None] == jnp.arange(experts, dtype=jnp.int32)[None, :]).astype(
        jnp.int32
    )
    slot_rank = jnp.sum((jnp.cumsum(one_hot, axis=0) - one_hot) * one_hot, axis=1)
    owner = flat_routes // exp_dev
    local = flat_routes - owner * exp_dev
    return owner * block_rows + local * capacity + slot_rank


MESH = pl.DeviceIdType.MESH


def exchange_kernel(
    capacity,
    outgoing,
    mix_part,
    gate_hbm,
    up_hbm,
    down_hbm,
    returned,
    projected,
    arrived,
    part,
    core_in,
    chip_sum,
    cross_in,
    final,
    gate,
    up,
    down,
    mix_held,
    mix_core,
    mix_sum,
    mix_cross,
    local_sem,
    dis_send,
    dis_recv,
    y1_send,
    y1_recv,
    c1_send,
    c1_recv,
    c2_send,
    c2_recv,
    y2_send,
    y2_recv,
    ret_send,
    ret_recv,
    m1_send,
    m1_recv,
    m2_send,
    m2_recv,
):
    ep_size, tp_size, rows, width = arrived.shape
    exp_dev, _, ff_dev = gate.shape
    highs = tp_size // 2
    ep = lax.axis_index("ep")
    tp = lax.axis_index("tp")
    hi, lo = tp // 2, tp % 2
    other = 1 - lo

    def remote(src, dst, send, recv, to_ep, to_tp):
        return pltpu.make_async_remote_copy(
            src_ref=src,
            dst_ref=dst,
            send_sem=send,
            recv_sem=recv,
            device_id=(to_ep, to_tp),
            device_id_type=MESH,
        )

    def peer_high(k):
        return lax.rem(hi + k, highs)

    def offset_of(i):
        far = jnp.where(i < 2, 2 * i + 1, ep_size + 1 - i)
        return jnp.where(i < ep_size - 2, far, 2 * (ep_size - 1 - i))

    def partner_ep(d):
        low = d
        mine = ep
        value = ep * 0
        bit = 1
        while bit < ep_size:
            a = (mine // bit) % 2
            b = (low // bit) % 2
            value = value + bit * ((a + b) % 2)
            bit *= 2
        return value

    def dispatch(d):
        peer = partner_ep(d)
        return remote(
            outgoing.at[peer], arrived.at[d, tp], dis_send.at[d], dis_recv.at[d], peer, tp
        )

    def gather_cross(d, k):
        high = peer_high(k)
        return remote(
            arrived.at[d, tp],
            arrived.at[d, tp],
            y1_send.at[d, k],
            y1_recv.at[d, highs - k],
            ep,
            high * 2 + lo,
        )

    def gather_cross_in(d, k):
        high = peer_high(k)
        return remote(
            arrived.at[d, high * 2 + lo],
            arrived.at[d, high * 2 + lo],
            y1_send.at[d, k],
            y1_recv.at[d, k],
            ep,
            high * 2 + lo,
        )

    def gather_core(d, high):
        slot = arrived.at[d, high * 2 + lo]
        return remote(slot, slot, c1_send.at[d, high], c1_recv.at[d, high], ep, hi * 2 + other)

    def gather_core_in(d, high):
        slot = arrived.at[d, high * 2 + other]
        return remote(slot, slot, c1_send.at[d, high], c1_recv.at[d, high], ep, hi * 2 + other)

    def reduce_core(d, high):
        return remote(
            part.at[high * 2 + other],
            core_in.at[d, high],
            c2_send.at[d, high],
            c2_recv.at[d, high],
            ep,
            hi * 2 + other,
        )

    def reduce_cross(d, k):
        high = peer_high(k)
        return remote(
            chip_sum.at[high],
            cross_in.at[d, highs - k - 1],
            y2_send.at[d, k],
            y2_recv.at[d, highs - k],
            ep,
            high * 2 + lo,
        )

    def reduce_cross_in(d, k):
        high = peer_high(k)
        return remote(
            chip_sum.at[high],
            cross_in.at[d, k - 1],
            y2_send.at[d, k],
            y2_recv.at[d, k],
            ep,
            high * 2 + lo,
        )

    def give_back(d):
        peer = partner_ep(d)
        return remote(final.at[d], returned.at[ep], ret_send.at[d], ret_recv.at[d], peer, tp)

    def give_back_in(d):
        peer = partner_ep(d)
        return remote(final.at[d], returned.at[peer], ret_send.at[d], ret_recv.at[d], peer, tp)

    def mix_core_copy(high):
        return remote(
            mix_held.at[high * 2 + other],
            mix_core.at[high],
            m1_send.at[high],
            m1_recv.at[high],
            ep,
            hi * 2 + other,
        )

    def mix_cross_copy(k):
        high = peer_high(k)
        return remote(
            mix_sum.at[high],
            mix_cross.at[highs - k - 1],
            m2_send.at[k],
            m2_recv.at[highs - k],
            ep,
            high * 2 + lo,
        )

    def mix_cross_in(k):
        high = peer_high(k)
        return remote(
            mix_sum.at[high],
            mix_cross.at[k - 1],
            m2_send.at[k],
            m2_recv.at[k],
            ep,
            high * 2 + lo,
        )

    own_rows = pltpu.make_async_copy(outgoing.at[ep], arrived.at[0, tp], local_sem.at[0])
    own_mix = pltpu.make_async_copy(mix_part, mix_held, local_sem.at[1])
    weight_copies = [
        pltpu.make_async_copy(gate_hbm, gate, local_sem.at[2]),
        pltpu.make_async_copy(up_hbm, up, local_sem.at[3]),
        pltpu.make_async_copy(down_hbm, down, local_sem.at[4]),
    ]
    own_rows.start()
    own_mix.start()
    for copy in weight_copies:
        copy.start()

    barrier = pltpu.get_barrier_semaphore()

    def greet(d, carry):
        pl.semaphore_signal(barrier, inc=1, device_id=(partner_ep(d), tp), device_id_type=MESH)
        return carry

    lax.fori_loop(1, ep_size, greet, 0)
    for k in range(1, highs):
        pl.semaphore_signal(
            barrier, inc=1, device_id=(ep, peer_high(k) * 2 + lo), device_id_type=MESH
        )
    pl.semaphore_signal(barrier, inc=1, device_id=(ep, hi * 2 + other), device_id_type=MESH)
    pl.semaphore_wait(barrier, ep_size - 1 + highs)

    def send_out(i, carry):
        dispatch(offset_of(i)).start()
        return carry

    lax.fori_loop(0, ep_size - 1, send_out, 0)

    def stage_a(d):
        for k in range(1, highs):
            gather_cross(d, k).start()
        gather_core(d, hi).start()

    own_rows.wait()
    stage_a(0)

    own_mix.wait()
    for high in range(highs):
        mix_core_copy(high).start()
    for high in range(highs):
        mix_core_copy(high).wait_recv()
    for high in range(highs):
        mix_sum[high] = (
            mix_held[high * 2 + lo].astype(jnp.float32) + mix_core[high].astype(jnp.float32)
        ).astype(jnp.bfloat16)
    for k in range(1, highs):
        mix_cross_copy(k).start()
    first = offset_of(ep * 0)
    dispatch(first).wait_recv()
    stage_a(first)
    for copy in weight_copies:
        copy.wait()

    row_expert = (
        lax.rem(lax.broadcasted_iota(jnp.int32, (tp_size * rows, 1), 0), rows) // capacity
    )
    column_step = min(width, 512)

    def step(i, carry):
        @pl.when(i + 1 < ep_size - 1)
        def _():
            d = offset_of(i + 1)
            dispatch(d).wait_recv()
            stage_a(d)

        @pl.when(i < ep_size)
        def _():
            d = offset_of(i)
            for k in range(1, highs):
                gather_cross_in(d, k).wait_recv()
                gather_core(d, peer_high(k)).start()

        @pl.when(i >= 2)
        def _():
            d = offset_of(i - 2)
            total = chip_sum[hi].astype(jnp.float32)
            for k in range(1, highs):
                reduce_cross(d, k).wait_send()
                reduce_cross_in(d, k).wait_recv()
                total = total + cross_in[d, k - 1].astype(jnp.float32)
            final[d] = total.astype(jnp.bfloat16)

            @pl.when(i == ep_size + 1)
            def _():
                pltpu.make_async_copy(final.at[0], returned.at[ep], local_sem.at[0]).start()

            @pl.when(i <= ep_size)
            def _():
                give_back(d).start()

        @pl.when((i >= 1) & (i <= ep_size))
        def _():
            d = offset_of(i - 1)
            for high in range(highs):
                reduce_core(d, high).wait_recv()
                reduce_core(d, high).wait_send()
                chip_sum[high] = (
                    part[high * 2 + lo].astype(jnp.float32) + core_in[d, high].astype(jnp.float32)
                ).astype(jnp.bfloat16)
            for k in range(1, highs):
                reduce_cross(d, k).start()

        @pl.when(i < ep_size)
        def _():
            d = offset_of(i)
            for high in range(highs):
                gather_core_in(d, high).wait_recv()
            hidden = []
            for e in range(exp_dev):
                block = arrived[d].reshape(tp_size * rows, width)
                gate_act = jnp.dot(block, gate[e], preferred_element_type=jnp.float32)
                up_act = jnp.dot(block, up[e], preferred_element_type=jnp.float32)
                act = gate_act / (1.0 + jnp.exp(-gate_act)) * up_act
                hidden.append(jnp.where(row_expert == e, act, 0.0).astype(jnp.bfloat16))
            joined = jnp.concatenate(hidden, axis=1)
            for start in range(0, width, column_step):
                columns = slice(start, start + column_step)
                out = jnp.dot(
                    joined,
                    down[:, :, columns].reshape(exp_dev * ff_dev, column_step),
                    preferred_element_type=jnp.float32,
                )
                part[:, :, columns] = out.astype(jnp.bfloat16).reshape(tp_size, rows, column_step)
            for high in range(highs):
                reduce_core(d, high).start()

        return carry

    lax.fori_loop(0, ep_size + 2, step, 0)

    total = mix_sum[hi].astype(jnp.float32)
    for k in range(1, highs):
        mix_cross_in(k).wait_recv()
        total = total + mix_cross[k - 1].astype(jnp.float32)
    projected[...] = total
    for k in range(1, highs):
        mix_cross_copy(k).wait_send()
    for high in range(highs):
        mix_core_copy(high).wait_send()

    def drain_all(d, carry):
        for k in range(1, highs):
            gather_cross(d, k).wait_send()
        for high in range(highs):
            gather_core(d, high).wait_send()
        return carry

    lax.fori_loop(0, ep_size, drain_all, 0)

    def drain(i, carry):
        d = offset_of(i)
        dispatch(d).wait_send()
        give_back(d).wait_send()
        give_back_in(d).wait_recv()
        return carry

    lax.fori_loop(0, ep_size - 1, drain, 0)
    pltpu.make_async_copy(final.at[0], returned.at[ep], local_sem.at[0]).wait()


def exchange(outgoing, mix_part, gate_weight, up_weight, down_weight, capacity):
    ep_size, rows, width = outgoing.shape
    tp_size, mix_rows, _ = mix_part.shape
    highs = tp_size // 2
    bf16 = jnp.bfloat16
    any_spec = pl.BlockSpec(memory_space=pl.ANY)
    dma = pltpu.SemaphoreType.DMA
    pair = (ep_size, highs)
    flops = 6 * gate_weight.size * ep_size * tp_size * rows
    return pl.pallas_call(
        functools.partial(exchange_kernel, capacity),
        out_shape=(
            jax.ShapeDtypeStruct(outgoing.shape, bf16),
            jax.ShapeDtypeStruct((mix_rows, width), jnp.float32),
        ),
        in_specs=[any_spec] * 5,
        out_specs=(any_spec, pl.BlockSpec(memory_space=pltpu.VMEM)),
        scratch_shapes=[
            pltpu.VMEM((ep_size, tp_size, rows, width), bf16),
            pltpu.VMEM((tp_size, rows, width), bf16),
            pltpu.VMEM((ep_size, highs, rows, width), bf16),
            pltpu.VMEM((highs, rows, width), bf16),
            pltpu.VMEM((ep_size, highs - 1, rows, width), bf16),
            pltpu.VMEM((ep_size, rows, width), bf16),
            pltpu.VMEM(gate_weight.shape, bf16),
            pltpu.VMEM(up_weight.shape, bf16),
            pltpu.VMEM(down_weight.shape, bf16),
            pltpu.VMEM(mix_part.shape, bf16),
            pltpu.VMEM((highs, mix_rows, width), bf16),
            pltpu.VMEM((highs, mix_rows, width), bf16),
            pltpu.VMEM((highs - 1, mix_rows, width), bf16),
            dma((5,)),
            dma((ep_size,)),
            dma((ep_size,)),
            dma(pair),
            dma(pair),
            dma(pair),
            dma(pair),
            dma(pair),
            dma(pair),
            dma(pair),
            dma(pair),
            dma((ep_size,)),
            dma((ep_size,)),
            dma((highs,)),
            dma((highs,)),
            dma((highs,)),
            dma((highs,)),
        ],
        compiler_params=pltpu.CompilerParams(
            collective_id=0, has_side_effects=True, vmem_limit_bytes=60 * 1024 * 1024
        ),
        cost_estimate=pl.CostEstimate(
            flops=flops, bytes_accessed=4 * outgoing.size, transcendentals=0
        ),
    )(outgoing, mix_part, gate_weight, up_weight, down_weight)


def on_device(
    pool_input,
    group_weight,
    pool_scale,
    out_weight,
    mix_gain,
    expert_input,
    routes,
    route_weights,
    moe_in_gain,
    gate_weight,
    up_weight,
    down_weight,
    moe_out_gain,
):
    tp_size = lax.axis_size("tp")
    ep_size = lax.axis_size("ep")
    tp_index = lax.axis_index("tp")
    rows_a = pool_input.shape[0]
    model_width = out_weight.shape[1]
    history_rows = 2**tp_size
    window = jnp.left_shift(jnp.int32(2), tp_index)
    history = passed_along(pool_input[rows_a - history_rows :], "ep", 1)
    extended = jnp.concatenate([history, pool_input], axis=0).astype(jnp.float32)
    running = jnp.cumsum(extended, axis=0)
    lagged = lax.dynamic_slice_in_dim(running, history_rows - window, rows_a, 0)
    current = running[history_rows:]
    position = lax.axis_index("ep") * rows_a + jnp.arange(rows_a, dtype=jnp.int32)
    divisor = jnp.minimum(position + 1, window).astype(jnp.float32)[:, None]
    pooled = ((current - lagged) / divisor - extended[history_rows:]).astype(jnp.bfloat16)
    grouped = (
        jnp.dot(pooled, group_weight[0], preferred_element_type=jnp.float32) * pool_scale
    ).astype(jnp.bfloat16)
    exp_dev = gate_weight.shape[0]
    experts = exp_dev * ep_size
    tok_dev = expert_input.shape[0]
    top_count = routes.shape[1]
    capacity = max(2, 5 * tok_dev * top_count // (4 * experts))
    block_rows = -(-exp_dev * capacity // 16) * 16
    slots_total = ep_size * block_rows
    normed = rms_scale(expert_input.astype(jnp.float32), moe_in_gain).astype(jnp.bfloat16)
    own_routes = lax.dynamic_slice_in_dim(routes, tp_index * tok_dev, tok_dev, 0)
    own_slots = slot_numbers(own_routes, experts, capacity, exp_dev, block_rows)
    slot_pairs = own_slots.reshape(tok_dev, top_count)
    slot_range = jnp.arange(slots_total, dtype=jnp.int32)
    chosen = slot_pairs[:, 0][None, :] == slot_range[:, None]
    for k in range(1, top_count):
        chosen = chosen | (slot_pairs[:, k][None, :] == slot_range[:, None])
    outgoing = (
        jnp.dot(chosen.astype(jnp.bfloat16), normed, preferred_element_type=jnp.float32)
        .astype(jnp.bfloat16)
        .reshape(ep_size, block_rows, model_width)
    )
    mix_part = (
        jnp.dot(grouped, out_weight, preferred_element_type=jnp.float32)
        .astype(jnp.bfloat16)
        .reshape(tp_size, rows_a // tp_size, model_width)
    )
    returned, projected = exchange(
        outgoing, mix_part, gate_weight, up_weight, down_weight, capacity
    )
    mixer_out = rms_scale(projected, mix_gain).astype(jnp.bfloat16)
    back = returned.reshape(slots_total, model_width)
    own_weights = lax.dynamic_slice_in_dim(route_weights, tp_index * tok_dev, tok_dev, 0)
    combined = jnp.zeros((tok_dev, model_width), jnp.float32)
    for k in range(top_count):
        place = (slot_pairs[:, k : k + 1] == slot_range[None, :]).astype(jnp.bfloat16)
        picked = jnp.dot(place, back, preferred_element_type=jnp.float32)
        combined = combined + picked * own_weights[:, k : k + 1]
    moe_out = rms_scale(combined, moe_out_gain).astype(jnp.bfloat16)
    return (mixer_out, moe_out)


def solution(mesh):
    in_specs = (
        P("ep", "tp"),
        P("tp", None, None),
        P("tp"),
        P("tp", None),
        P(),
        P(("ep", "tp"), None),
        P("ep", None),
        P("ep", None),
        P(),
        P("ep", None, "tp"),
        P("ep", None, "tp"),
        P("ep", "tp", None),
        P(),
    )
    out_specs = (P(("ep", "tp"), None), P(("ep", "tp"), None))
    return jax.shard_map(
        on_device, mesh=mesh, in_specs=in_specs, out_specs=out_specs, check_vma=False
    )
```
